32 devices in a mesh: kv: 4 (over y, x), tp: 8 (over z, core).
Axes of the slice: x: 2, y: 2, z: 4, core: 2. Of those that a mesh axis runs over, the one named last changes fastest.
Arguments:
- tokens: bfloat16 [16, 4096], P(None, ('kv', 'tp')), may hold values from -9 to 9
- lengths: int32 [16], replicated, may hold values from 1 to 4096, 16384 in all
- gain_attn: float32 [4096], P('kv'), may hold values from 0.1 to 1.9
- w_query_nope: bfloat16 [4096, 4096], P('kv', 'tp'), may hold values from -0.09375 to 0.09375
- w_query_rope: bfloat16 [4096, 2048], P('kv', 'tp'), may hold values from -0.09375 to 0.09375
- w_latent: bfloat16 [4096, 512], P('kv'), may hold values from -0.09375 to 0.09375
- w_rope_key: bfloat16 [4096, 64], P('kv'), may hold values from -0.09375 to 0.09375
- gain_latent: float32 [512], replicated, may hold values from 0.1 to 1.9
- w_key_up: bfloat16 [512, 4096], P(None, 'tp'), may hold values from -0.75 to 0.75
- w_value_up: bfloat16 [512, 4096], P(None, 'tp'), may hold values from -0.25 to 0.25
- w_out: bfloat16 [4096, 4096], P('tp', 'kv'), may hold values from -0.25 to 0.25
- gain_mlp: float32 [4096], P('kv'), may hold values from 0.1 to 1.9
- w_up: bfloat16 [4096, 16384], P('kv', 'tp'), may hold values from -0.09375 to 0.09375
- w_down: bfloat16 [16384, 4096], P('tp', 'kv'), may hold values from -0.046875 to 0.046875
- cache_latent: bfloat16 [16, 4096, 512], P('tp', 'kv'), may hold values from -6 to 6
- cache_rope: bfloat16 [16, 4096, 64], P('tp', 'kv'), may hold values from -900 to 900
Outputs:
- mixed: bfloat16 [16, 4096], P(None, ('kv', 'tp'))
The draws below stay inside these ranges and needn't reach their ends.
Inputs may be any that keep to these rules, and one draw needn't show every extreme that they name: `lengths`: one sequence has exactly 4096 live positions.
All inputs are finite; a program needn't handle non-finite values.
Results may differ from the reference program's by a relative error of at most 0.035.
The reference program's roundings to bfloat16 on the way count: a program that leaves them out, or rounds other values in their place, can miss the bound.
Values may be sent and summed in bfloat16 or wider, within the bound.
A program may use at most 64 MiB of HBM per device.

```python
import math
import jax
import jax.numpy as jnp
import numpy as np
from jax import lax

D = 4096
H = 32
NOPE = 128
ROPE = 64
VD = 128
RANK = 512
FF = 16384
CACHE_DEV = 1024
BATCH = 16
CACHE = 4096
N_KV = 4


def draw_tokens(key, part):
    column_scale = 0.5 * 3.0 ** (jnp.arange(D, dtype=jnp.float32) / D)
    values = jnp.clip(jax.random.normal(key, (BATCH, D), jnp.float32), -6.0, 6.0)
    return (values * column_scale).astype(jnp.bfloat16)


def draw_cache_rope(key, part):
    values = jnp.clip(jax.random.normal(key, (BATCH, CACHE, ROPE), jnp.float32), -6.0, 6.0)
    return values.astype(jnp.bfloat16)


def block_levels(key, shape, split, low, top_value):
    def one(position, shards_of):
        heights = jax.random.uniform(jax.random.fold_in(jax.random.fold_in(key, 6), position), (shards_of,), jnp.float32, low / len(split), top_value / len(split))
        return jnp.repeat(jnp.exp(heights), shape[position] // shards_of).reshape((-1,) + (1,) * (len(shape) - position - 1))

    level = one(*split[0])
    for cut in split[1:]:
        level = level * one(*cut)
    return level


def profile(count, total, limit, lean):
    portions = [(1 << 20) // math.isqrt(grade ** lean) + 1 for grade in range(2, count + 1)]
    surplus, counts = total - limit - (count - 1), [1] * (count - 1)
    while surplus > 0:
        candidates = [i for i in range(count - 1) if counts[i] < limit]
        mass, left = sum([portions[i] for i in candidates]), surplus
        for i in candidates:
            addition = min(limit - counts[i], max(1, left * portions[i] // mass), surplus)
            counts[i] = counts[i] + addition
            surplus = surplus - addition
    return np.array([limit] + counts)


def uneven_parts(rng, count, total, limit, skew):
    if count == 2:
        one = jax.random.randint(rng, (), max(1, total - limit), min(limit, total - 1) + 1)
        return jnp.stack([one, total - one])
    sizes = jnp.asarray(profile(count, total, limit, skew), jnp.int32)
    pairs = (count - 1) // 2
    source_of, sink = sizes[1:1 + 2 * pairs:2], sizes[2:2 + 2 * pairs:2]
    room = jnp.minimum(source_of - 1, limit - sink)
    moved = jax.random.randint(jax.random.fold_in(rng, 1), (pairs,), 0, 1 << 20) % (room + 1)
    sizes = sizes.at[1:1 + 2 * pairs:2].set(source_of - moved).at[2:2 + 2 * pairs:2].set(sink + moved)
    return sizes[jax.random.permutation(jax.random.fold_in(rng, 2), count)]


def centred(stream_key, dims, deviation, limit, shards=(), kind=jnp.bfloat16):
    values = jax.random.normal(stream_key, dims, jnp.float32) * deviation
    if len(shards) > 0:
        values = block_levels(stream_key, dims, shards, -0.22, 0.18) * values
    return jnp.clip(values, min=-limit, max=limit).astype(kind)


def setup_inputs(seed: int = 0) -> dict:
    arg_keys = jax.random.split(jax.random.key(seed), 17)
    tokens = draw_tokens(jax.random.fold_in(arg_keys[16], 71), 0)
    lengths = uneven_parts(arg_keys[1], BATCH, BATCH * CACHE // 4, CACHE, 2).astype(jnp.int32)
    gain_attn = jnp.clip(1.0 + 0.18 * jax.random.normal(arg_keys[2], (D,), jnp.float32), 0.1, 1.9)
    w_query_nope = centred(arg_keys[3], (D, H * NOPE), D ** -0.5, 0.09375, ((0, 4), (1, 8)))
    w_query_rope = centred(arg_keys[4], (D, H * ROPE), D ** -0.5, 0.09375, ((0, 4), (1, 8)))
    w_latent = centred(arg_keys[5], (D, RANK), D ** -0.5, 0.09375, ((0, 4),))
    w_rope_key = centred(arg_keys[6], (D, ROPE), D ** -0.5, 0.09375, ((0, 4),))
    gain_latent = jnp.clip(1.0 + 0.18 * jax.random.normal(arg_keys[7], (RANK,), jnp.float32), 0.1, 1.9)
    w_key_up = centred(arg_keys[8], (RANK, H * NOPE), (RANK // 8) ** -0.5, 0.75, ((1, 8),))
    w_value_up = centred(arg_keys[9], (RANK, H * VD), RANK ** -0.5, 0.25, ((1, 8),))
    w_out = centred(arg_keys[10], (H * VD, D), (H * VD // 8) ** -0.5, 0.25, ((0, 8), (1, 4)))
    gain_mlp = jnp.clip(1.0 + 0.18 * jax.random.normal(arg_keys[11], (D,), jnp.float32), 0.1, 1.9)
    w_up = centred(arg_keys[12], (D, FF), D ** -0.5, 0.09375, ((0, 4), (1, 8)))
    w_down = centred(arg_keys[13], (FF, D), FF ** -0.5, 0.046875, ((0, 8), (1, 4)))
    cache_latent = centred(arg_keys[14], (BATCH, CACHE, RANK), 1.0, 6.0, ((0, 8), (1, 4)))
    cache_rope = draw_cache_rope(jax.random.fold_in(arg_keys[16], 71), 0)
    return {"tokens": tokens, "lengths": lengths, "gain_attn": gain_attn, "w_query_nope": w_query_nope, "w_query_rope": w_query_rope, "w_latent": w_latent, "w_rope_key": w_rope_key, "gain_latent": gain_latent, "w_key_up": w_key_up, "w_value_up": w_value_up, "w_out": w_out, "gain_mlp": gain_mlp, "w_up": w_up, "w_down": w_down, "cache_latent": cache_latent, "cache_rope": cache_rope}


EPS = 1e-06

def rotate(values, positions):
    half_dim = values.shape[-1] // 2
    inv_freq = 10000.0 ** (-jnp.arange(half_dim, dtype=jnp.float32) / half_dim)
    angles = positions.astype(jnp.float32)[..., None] * inv_freq
    cos_part = jnp.cos(angles)
    sin_part = jnp.sin(angles)
    lower = values[..., :half_dim]
    upper = values[..., half_dim:]
    return jnp.concatenate([lower * cos_part - upper * sin_part, upper * cos_part + lower * sin_part], axis=-1)

def reference(tokens, lengths, gain_attn, w_query_nope, w_query_rope, w_latent, w_rope_key, gain_latent, w_key_up, w_value_up, w_out, gain_mlp, w_up, w_down, cache_latent, cache_rope):
    batch_rows = tokens.shape[0]
    widened = tokens.astype(jnp.float32)
    inv_rms = lax.rsqrt(lax.optimization_barrier(jnp.mean(widened * widened, axis=1)) + EPS)
    scaled = (widened * gain_attn.astype(jnp.float32)).astype(jnp.bfloat16)
    q_nope = (jnp.dot(scaled, w_query_nope, preferred_element_type=jnp.float32) * inv_rms[:, None]).astype(jnp.bfloat16).reshape(batch_rows, H, NOPE)
    rope_raw = (jnp.dot(scaled, w_query_rope, preferred_element_type=jnp.float32) * inv_rms[:, None]).reshape(batch_rows, H, ROPE)
    q_rope = rotate(rope_raw, lengths[:, None]).astype(jnp.bfloat16)
    raw_latent = jnp.dot(scaled, w_latent, preferred_element_type=jnp.float32) * inv_rms[:, None]
    latent_new = (raw_latent * lax.rsqrt(lax.optimization_barrier(jnp.mean(raw_latent * raw_latent, axis=1, keepdims=True)) + EPS) * gain_latent.astype(jnp.float32)).astype(jnp.bfloat16)
    key_new = rotate(jnp.dot(scaled, w_rope_key, preferred_element_type=jnp.float32) * inv_rms[:, None], lengths).astype(jnp.bfloat16)
    key_up = w_key_up.reshape(RANK, H, NOPE).astype(jnp.float32)
    q_latent = jnp.einsum('bhn,rhn->bhr', q_nope.astype(jnp.float32), key_up).astype(jnp.bfloat16)
    score_scale = (NOPE + ROPE) ** (-0.5)

    def attend(sequence_data):
        latent_query, rope_query, latent_rows, rope_rows, live_len, own_latent, own_key = sequence_data
        positions = jnp.arange(CACHE, dtype=jnp.int32)
        rotated = rotate(rope_rows.astype(jnp.float32), positions).astype(jnp.bfloat16)
        scores = (jnp.dot(latent_query, latent_rows.T, preferred_element_type=jnp.float32) + jnp.dot(rope_query, rotated.T, preferred_element_type=jnp.float32)) * score_scale
        live_mask = (positions < live_len).reshape(N_KV, CACHE_DEV)
        blocks = scores.reshape(H, N_KV, CACHE_DEV)
        block_max = lax.optimization_barrier(jnp.max(jnp.where(live_mask[None], blocks, -1e+30), axis=2))
        exponent = jnp.where(live_mask[None], jnp.exp(blocks - block_max[..., None]), 0.0)
        block_sum = lax.optimization_barrier(jnp.sum(exponent, axis=2))
        expo_low = lax.optimization_barrier(exponent.astype(jnp.bfloat16))
        weighted = jnp.einsum('hjp,jpr->hjr', expo_low.astype(jnp.float32), latent_rows.reshape(N_KV, CACHE_DEV, RANK).astype(jnp.float32))
        block_out = lax.optimization_barrier((weighted / jnp.where(block_sum > 0, block_sum, 1.0)[..., None]).astype(jnp.bfloat16))
        own_score = (jnp.dot(latent_query, own_latent, preferred_element_type=jnp.float32) + jnp.dot(rope_query, own_key, preferred_element_type=jnp.float32)) * score_scale
        new_max = jnp.maximum(lax.optimization_barrier(jnp.max(block_max, axis=1)), own_score)
        block_weight = block_sum * jnp.exp(block_max - new_max[:, None])
        own_weight = jnp.exp(own_score - new_max)
        result = (lax.optimization_barrier(jnp.sum(block_weight[..., None] * block_out.astype(jnp.float32), axis=1)) + own_weight[:, None] * own_latent.astype(jnp.float32)[None, :]) / (lax.optimization_barrier(jnp.sum(block_weight, axis=1)) + own_weight)[:, None]
        return result.astype(jnp.bfloat16)
    o_latent = lax.map(attend, (q_latent, q_rope, cache_latent, cache_rope, lengths, latent_new, key_new))
    value_up = w_value_up.reshape(RANK, H, VD).astype(jnp.float32)
    head_out = jnp.einsum('bhr,rhv->bhv', o_latent.astype(jnp.float32), value_up).astype(jnp.bfloat16).reshape(batch_rows, H * VD)
    resid = (widened + jnp.dot(head_out, w_out, preferred_element_type=jnp.float32)).astype(jnp.bfloat16)
    resid_wide = resid.astype(jnp.float32)
    inv_rms2 = lax.rsqrt(lax.optimization_barrier(jnp.mean(resid_wide * resid_wide, axis=1)) + EPS)
    scaled2 = (resid_wide * gain_mlp.astype(jnp.float32)).astype(jnp.bfloat16)
    up_sum = jnp.dot(scaled2, w_up, preferred_element_type=jnp.float32)
    activated = jnp.square(jnp.maximum(up_sum, 0.0)).astype(jnp.bfloat16)
    down_sum = jnp.dot(activated, w_down, preferred_element_type=jnp.float32)
    return (resid_wide + (inv_rms2 * inv_rms2)[:, None] * down_sum).astype(jnp.bfloat16)
```

```python
import functools

import jax
import jax.numpy as jnp
import numpy as np
from jax import lax
from jax.experimental import pallas as pl
from jax.experimental.pallas import tpu as pltpu
from jax.sharding import PartitionSpec as P

D = 4096
NOPE = 128
ROPE = 64
VD = 128
RANK = 512


EPS = 1e-06


def merged_2(value, axis, combine):
    everything = jax.tree.map(
        lambda part, kind: lax.all_gather(part.astype(kind), axis),
        value,
        (jnp.bfloat16, jnp.bfloat16, jnp.bfloat16),
    )

    def take(k):
        return jax.tree.map(lambda part, own: part[k].astype(own.dtype), everything, value)

    return lax.fori_loop(
        1, lax.axis_size(axis), lambda k, so_far: combine(so_far, take(k)), take(0)
    )


def rotate(values, positions):
    half_dim = values.shape[-1] // 2
    inv_freq = 10000.0 ** (-jnp.arange(half_dim, dtype=jnp.float32) / half_dim)
    angles = positions.astype(jnp.float32)[..., None] * inv_freq
    cos_part = jnp.cos(angles)
    sin_part = jnp.sin(angles)
    lower = values[..., :half_dim]
    upper = values[..., half_dim:]
    return jnp.concatenate(
        [lower * cos_part - upper * sin_part, upper * cos_part + lower * sin_part], axis=-1
    )


def combine(earlier, later):
    max_one, sum_one, out_one = earlier
    max_two, sum_two, out_two = later
    new_max = jnp.maximum(max_one, max_two)
    weight_one = sum_one * jnp.exp(max_one - new_max)
    weight_two = sum_two * jnp.exp(max_two - new_max)
    merged = weight_one + weight_two
    safe_sum = jnp.where(merged > 0, merged, 1.0)
    result = (
        weight_one[..., None] * out_one.astype(jnp.float32)
        + weight_two[..., None] * out_two.astype(jnp.float32)
    ) / safe_sum[..., None]
    return (new_max, merged, result.astype(jnp.bfloat16))


def per_device(
    tokens,
    lengths,
    gain_attn,
    w_query_nope,
    w_query_rope,
    w_latent,
    w_rope_key,
    gain_latent,
    w_key_up,
    w_value_up,
    w_out,
    gain_mlp,
    w_up,
    w_down,
    cache_latent,
    cache_rope,
):
    kv_index = lax.axis_index("kv")
    tp_index = lax.axis_index("tp")
    seq_dev = cache_latent.shape[0]
    cache_dev = cache_latent.shape[1]
    heads_dev = w_key_up.shape[1] // NOPE
    block_cols = lax.all_gather(tokens, "tp", axis=1, tiled=True)
    batch_rows = block_cols.shape[0]
    widened = block_cols.astype(jnp.float32)
    square_piece = jnp.sum(widened * widened, axis=1)
    scaled = (widened * gain_attn).astype(jnp.bfloat16)
    part_nope = jnp.dot(scaled, w_query_nope, preferred_element_type=jnp.float32)
    part_rope = jnp.dot(scaled, w_query_rope, preferred_element_type=jnp.float32)
    own_rows = lax.dynamic_slice_in_dim(scaled, tp_index * seq_dev, seq_dev, 0)
    part_latent = jnp.dot(own_rows, w_latent, preferred_element_type=jnp.float32)
    part_key = jnp.dot(own_rows, w_rope_key, preferred_element_type=jnp.float32)
    square_sum, nope_sum, rope_sum, latent_sum, key_sum = lax.psum(
        (square_piece, part_nope, part_rope, part_latent, part_key), "kv"
    )
    inv_rms = lax.rsqrt(square_sum / D + EPS)
    q_nope = (nope_sum * inv_rms[:, None]).astype(jnp.bfloat16).reshape(batch_rows, heads_dev, NOPE)
    rope_raw = (rope_sum * inv_rms[:, None]).reshape(batch_rows, heads_dev, ROPE)
    q_rope = rotate(rope_raw, lengths[:, None]).astype(jnp.bfloat16)
    key_up = w_key_up.reshape(RANK, heads_dev, NOPE)
    q_latent = jnp.einsum(
        "bhn,rhn->bhr", q_nope, key_up, preferred_element_type=jnp.float32
    ).astype(jnp.bfloat16)
    latent_query, rope_query = (
        lax.all_to_all(q_latent, "tp", split_axis=0, concat_axis=1, tiled=True),
        lax.all_to_all(q_rope, "tp", split_axis=0, concat_axis=1, tiled=True),
    )
    own_inv = lax.dynamic_slice_in_dim(inv_rms, tp_index * seq_dev, seq_dev, 0)
    own_len = lax.dynamic_slice_in_dim(lengths, tp_index * seq_dev, seq_dev, 0)
    raw_latent = latent_sum * own_inv[:, None]
    latent_new = (
        raw_latent
        * lax.rsqrt(jnp.mean(raw_latent * raw_latent, axis=1, keepdims=True) + EPS)
        * gain_latent
    ).astype(jnp.bfloat16)
    key_new = rotate(key_sum * own_inv[:, None], own_len).astype(jnp.bfloat16)
    score_scale = (NOPE + ROPE) ** (-0.5)
    positions = kv_index * cache_dev + jnp.arange(cache_dev, dtype=jnp.int32)
    rotated = rotate(cache_rope.astype(jnp.float32), positions).astype(jnp.bfloat16)
    scores = (
        jnp.einsum("shr,spr->shp", latent_query, cache_latent, preferred_element_type=jnp.float32)
        + jnp.einsum("shk,spk->shp", rope_query, rotated, preferred_element_type=jnp.float32)
    ) * score_scale
    live_mask = positions[None, None, :] < own_len[:, None, None]
    block_max = jnp.max(jnp.where(live_mask, scores, -1e30), axis=2)
    exponent = jnp.where(live_mask, jnp.exp(scores - block_max[..., None]), 0.0)
    block_sum = jnp.sum(exponent, axis=2)
    weighted = jnp.einsum(
        "shp,spr->shr",
        exponent.astype(jnp.bfloat16),
        cache_latent,
        preferred_element_type=jnp.float32,
    )
    block_out = (weighted / jnp.where(block_sum > 0, block_sum, 1.0)[..., None]).astype(
        jnp.bfloat16
    )
    block_max, block_sum, block_out = merged_2((block_max, block_sum, block_out), "kv", combine)
    own_score = (
        jnp.einsum("shr,sr->sh", latent_query, latent_new, preferred_element_type=jnp.float32)
        + jnp.einsum("shk,sk->sh", rope_query, key_new, preferred_element_type=jnp.float32)
    ) * score_scale
    new_max = jnp.maximum(block_max, own_score)
    carried = block_sum * jnp.exp(block_max - new_max)
    own_weight = jnp.exp(own_score - new_max)
    o_latent = (
        (
            carried[..., None] * block_out.astype(jnp.float32)
            + own_weight[..., None] * latent_new.astype(jnp.float32)[:, None, :]
        )
        / (carried + own_weight)[..., None]
    ).astype(jnp.bfloat16)
    head_latent = lax.all_to_all(o_latent, "tp", split_axis=1, concat_axis=0, tiled=True)
    value_up = w_value_up.reshape(RANK, heads_dev, VD)
    head_out = (
        jnp.einsum("bhr,rhv->bhv", head_latent, value_up, preferred_element_type=jnp.float32)
        .astype(jnp.bfloat16)
        .reshape(batch_rows, heads_dev * VD)
    )
    attn_part = jnp.dot(head_out, w_out, preferred_element_type=jnp.float32)
    attn_sum = lax.psum(attn_part, "tp")
    resid = (widened + attn_sum).astype(jnp.bfloat16)
    resid_wide = resid.astype(jnp.float32)
    square_two = jnp.sum(resid_wide * resid_wide, axis=1)
    scaled2 = (resid_wide * gain_mlp).astype(jnp.bfloat16)
    up_part = jnp.dot(scaled2, w_up, preferred_element_type=jnp.float32)
    spread_squares = jnp.broadcast_to(square_two[:, None], (batch_rows, lax.axis_size("kv")))
    up_share, square_cols = (
        lax.psum_scatter(up_part, "kv", scatter_dimension=1, tiled=True),
        lax.psum_scatter(spread_squares, "kv", scatter_dimension=1, tiled=True),
    )
    square_all = square_cols[:, 0]
    active_share = jnp.square(jnp.maximum(up_share, 0.0)).astype(jnp.bfloat16)
    activated = lax.all_gather(active_share, "kv", axis=1, tiled=True)
    inv_rms2 = lax.rsqrt(square_all / D + EPS)
    down_part = jnp.dot(activated, w_down, preferred_element_type=jnp.float32)
    down_sum = lax.psum_scatter(down_part, "tp", scatter_dimension=1, tiled=True)
    out_cols = down_sum.shape[1]
    resid_cols = lax.dynamic_slice_in_dim(resid_wide, tp_index * out_cols, out_cols, 1)
    return (resid_cols + (inv_rms2 * inv_rms2)[:, None] * down_sum).astype(jnp.bfloat16)


MESH = pl.DeviceIdType.MESH
BF16 = jnp.bfloat16
F32 = jnp.float32
FINE = 32


def dot(a, b):
    return jnp.dot(a, b, preferred_element_type=F32)


def dot_nt(a, b):
    return lax.dot_general(a, b, (((1,), (1,)), ((), ())), preferred_element_type=F32)


def iota(shape, axis):
    return lax.broadcasted_iota(jnp.int32, shape, axis)


def layer_kernel(
    n_kv,
    n_tp,
    len_ref,
    tok_ref,
    gain_attn,
    gain_latent,
    gain_mlp,
    coarse_ref,
    fine_ref,
    freq_ref,
    h_qn,
    h_qr,
    h_lat,
    h_key,
    h_kup,
    h_vup,
    h_out,
    h_up,
    h_down,
    h_cl,
    h_cr,
    out_ref,
    w_qn,
    w_qr,
    w_lat,
    w_key,
    w_kup,
    w_vup,
    w_out,
    w_up,
    w_down,
    c_lat,
    c_rope,
    rot,
    tok_all,
    qp_own,
    qp_in,
    lat_own,
    lat_in,
    sq_own,
    sq_in,
    q_own,
    q_in,
    bo_own,
    bo_in,
    st_own,
    st_in,
    o_own,
    o_in,
    ap_own,
    ap_in,
    res_own,
    res_all,
    up_own,
    up_in,
    sq2_own,
    sq2_in,
    act_own,
    act_all,
    dn_own,
    dn_in,
    load_sem,
    send_sem,
    recv_sem,
):
    kv = lax.axis_index("kv")
    tp = lax.axis_index("tp")
    size = {"kv": n_kv, "tp": n_tp}
    here = {"kv": kv, "tp": tp}
    batch, col = tok_ref.shape
    seqs, cache_dev, rank = c_lat.shape
    heads = w_kup.shape[1] // NOPE
    rows = batch * heads
    group = seqs * heads
    n_nope = heads * NOPE
    n_rope = heads * ROPE

    loads = {}
    order = (
        ("qn", h_qn, w_qn),
        ("qr", h_qr, w_qr),
        ("lat", h_lat, w_lat),
        ("key", h_key, w_key),
        ("cr", h_cr, c_rope),
        ("kup", h_kup, w_kup),
        ("cl", h_cl, c_lat),
        ("vup", h_vup, w_vup),
        ("out", h_out, w_out),
        ("up", h_up, w_up),
        ("down", h_down, w_down),
    )
    for i, (name, hbm, vmem) in enumerate(order):
        loads[name] = pltpu.make_async_copy(hbm, vmem, load_sem.at[i])
        loads[name].start()

    barrier = pltpu.get_barrier_semaphore()
    for axis in ("kv", "tp"):
        for d in range(1, size[axis]):
            pl.semaphore_signal(
                barrier,
                inc=1,
                device_id={axis: lax.rem(here[axis] + d, size[axis])},
                device_id_type=MESH,
            )

    started = []

    def send(axis, d, source, target):
        i = len(started)
        copy = pltpu.make_async_remote_copy(
            src_ref=source,
            dst_ref=target,
            send_sem=send_sem.at[i],
            recv_sem=recv_sem.at[i],
            device_id={axis: lax.rem(here[axis] + d, size[axis])},
            device_id_type=MESH,
        )
        copy.start()
        started.append(copy)
        return copy

    def peer(axis, d):
        return lax.rem(here[axis] + d, size[axis])

    def arrive(copies):
        for copy in copies:
            copy.wait_recv()

    lane_r = iota((batch, n_rope), 1)
    row_b = iota((batch, n_rope), 0)
    len_b = jnp.zeros((batch, n_rope), jnp.int32)
    for b in range(batch):
        len_b = jnp.where(row_b == b, len_ref[b], len_b)
    angle = len_b.astype(F32) * freq_ref[0:1, :n_rope]
    q_cos = jnp.cos(angle)
    q_sin = jnp.sin(angle)
    lane_k = iota((group, 128), 1)
    row_k = iota((group, 128), 0) // heads
    len_k = jnp.zeros((group, 128), jnp.int32)
    for s in range(seqs):
        len_k = jnp.where(row_k == s, len_ref[tp * seqs + s], len_k)
    angle_k = len_k.astype(F32) * freq_ref[0:1, :128]
    k_cos = jnp.cos(angle_k)
    k_sin = jnp.sin(angle_k)

    spread = (iota((rows, batch), 0) // heads == iota((rows, batch), 1)).astype(F32).astype(BF16)
    gather = (iota((batch, rows), 1) // heads == iota((batch, rows), 0)).astype(F32).astype(BF16)
    pick = (iota((group, batch), 0) // heads + tp * seqs == iota((group, batch), 1))
    pick = pick.astype(F32).astype(BF16)

    pl.semaphore_wait(barrier, n_kv + n_tp - 2)

    tok_copies = [send("tp", d, tok_ref, tok_all.at[tp]) for d in range(1, n_tp)]
    tok_all[tp] = tok_ref[...]

    loads["cr"].wait()
    half = ROPE // 2
    s_row = iota((ROPE, ROPE), 0)
    s_col = iota((ROPE, ROPE), 1)
    swap = jnp.where(s_row == s_col + half, -1.0, 0.0) + jnp.where(s_row + half == s_col, 1.0, 0.0)
    swap = swap.astype(BF16)
    n_coarse = cache_dev // FINE
    first = pl.multiple_of(kv * n_coarse, 8)
    cos_a = coarse_ref[0, pl.ds(first, n_coarse), :]
    sin_a = coarse_ref[1, pl.ds(first, n_coarse), :]
    cos_b = fine_ref[0]
    sin_b = fine_ref[1]
    for i in range(n_coarse):
        part = pl.ds(i * FINE, FINE)
        ca, sa = cos_a[i : i + 1], sin_a[i : i + 1]
        cos_p = ca * cos_b - sa * sin_b
        sin_p = sa * cos_b + ca * sin_b
        for s in range(seqs):
            keys = c_rope[s, part, :]
            turned = keys.astype(F32) * cos_p + dot(keys, swap) * sin_p
            rot[s, part, :] = turned.astype(BF16)

    arrive(tok_copies)
    toks = jnp.concatenate([tok_all[i] for i in range(n_tp)], axis=1)
    wide = toks.astype(F32)
    scaled = (wide * gain_attn[...]).astype(BF16)
    loads["qn"].wait()
    qp_own[:, :n_nope] = dot(scaled, w_qn[...]).astype(BF16)
    loads["qr"].wait()
    qp_own[:, n_nope:] = dot(scaled, w_qr[...]).astype(BF16)
    sq_own[...] = jnp.broadcast_to(jnp.sum(wide * wide, axis=1, keepdims=True), sq_own.shape)
    qp_copies = [send("kv", d, qp_own, qp_in.at[d - 1]) for d in range(1, n_kv)]
    sq_copies = [send("kv", d, sq_own, sq_in.at[d - 1]) for d in range(1, n_kv)]
    own_tok = dot(pick, toks)
    own_scaled = (own_tok * gain_attn[...]).astype(BF16)
    loads["lat"].wait()
    lat_own[:, :rank] = dot(own_scaled, w_lat[...])
    loads["key"].wait()
    lat_own[:, rank : rank + ROPE] = dot(own_scaled, w_key[...])
    lat_own[:, rank + ROPE :] = jnp.broadcast_to(
        jnp.sum(own_tok * own_tok, axis=1, keepdims=True), (group, ROPE)
    )
    lat_copies = [send("kv", d, lat_own, lat_in.at[d - 1]) for d in range(1, n_kv)]

    loads["kup"].wait()
    arrive(qp_copies)
    arrive(sq_copies)
    q_sum = qp_own[...].astype(F32)
    square = sq_own[:, 0:1]
    for d in range(n_kv - 1):
        q_sum = q_sum + qp_in[d].astype(F32)
        square = square + sq_in[d, :, 0:1]
    q_sum = q_sum * lax.rsqrt(square / D + EPS)
    q_nope = q_sum[:, :n_nope].astype(BF16)
    raw = q_sum[:, n_nope:]
    swapped = jnp.where(
        lane_r % ROPE < half, -pltpu.roll(raw, n_rope - half, 1), pltpu.roll(raw, half, 1)
    )
    q_rope = (raw * q_cos + swapped * q_sin).astype(BF16)
    own_cols = iota((rows, n_nope), 1) // NOPE == iota((rows, n_nope), 0) % heads
    own_rope = iota((rows, n_rope), 1) // ROPE == iota((rows, n_rope), 0) % heads
    q_wide = jnp.where(own_cols, dot(spread, q_nope), 0.0).astype(BF16)
    q_lat = dot_nt(q_wide, w_kup[...])
    r_wide = jnp.where(own_rope, dot(spread, q_rope), 0.0).astype(BF16)
    fold = (iota((n_rope, 128), 0) % ROPE == iota((n_rope, 128), 1)).astype(F32).astype(BF16)
    q_rot = dot(r_wide, fold)
    q_own[:, :, :rank] = q_lat.reshape(n_tp, group, rank).astype(BF16)
    q_own[:, :, rank:] = q_rot.reshape(n_tp, group, 128).astype(BF16)
    q_copies = [
        send("tp", d, q_own.at[peer("tp", d)], q_in.at[tp]) for d in range(1, n_tp)
    ]
    q_in[tp] = q_own[tp]

    arrive(lat_copies)
    lat_sum = lat_own[...]
    for d in range(n_kv - 1):
        lat_sum = lat_sum + lat_in[d]
    own_inv = lax.rsqrt(lat_sum[:, rank + ROPE : rank + ROPE + 1] / D + EPS)
    raw_latent = lat_sum[:, :rank] * own_inv
    mean_sq = jnp.mean(raw_latent * raw_latent, axis=1, keepdims=True)
    latent_new = (raw_latent * lax.rsqrt(mean_sq + EPS) * gain_latent[...]).astype(BF16).astype(F32)
    raw_key = lat_sum[:, rank:] * own_inv
    raw_key = jnp.where(lane_k < ROPE, raw_key, pltpu.roll(raw_key, ROPE, 1))
    swap_key = jnp.where(
        lane_k % ROPE < half, -pltpu.roll(raw_key, 128 - half, 1), pltpu.roll(raw_key, half, 1)
    )
    key_new = (raw_key * k_cos + swap_key * k_sin).astype(BF16).astype(F32)
    key_new = jnp.where(lane_k < ROPE, key_new, 0.0)
    latent_rows = jnp.broadcast_to(latent_new[None], (n_tp, group, rank)).reshape(rows, rank)
    key_rows = jnp.broadcast_to(key_new[None], (n_tp, group, 128)).reshape(rows, 128)

    row_seq = iota((rows, 1), 0) % group // heads
    own_len = jnp.zeros((rows, 1), jnp.int32)
    for s in range(seqs):
        own_len = jnp.where(row_seq == s, len_ref[tp * seqs + s], own_len)
    score_scale = (NOPE + ROPE) ** (-0.5)

    loads["cl"].wait()
    arrive(q_copies)
    q_all = q_in[...].astype(F32).reshape(rows, rank + 128)
    q_low = q_all.astype(BF16)
    latent_query = q_low[:, :rank]
    rope_query = q_low[:, rank : rank + ROPE]
    scores = None
    for s in range(seqs):
        one = dot_nt(latent_query, c_lat[s]) + dot_nt(rope_query, rot[s])
        scores = one if scores is None else jnp.where(row_seq == s, one, scores)
    scores = scores * score_scale
    live = kv * cache_dev + iota((rows, cache_dev), 1) < own_len
    block_max = jnp.max(jnp.where(live, scores, -1e30), axis=1, keepdims=True)
    expo = jnp.where(live, jnp.exp(scores - block_max), 0.0)
    block_sum = jnp.sum(expo, axis=1, keepdims=True)
    expo_low = expo.astype(BF16)
    weighted = None
    for s in range(seqs):
        one = dot(expo_low, c_lat[s])
        weighted = one if weighted is None else jnp.where(row_seq == s, one, weighted)
    bo_own[...] = (weighted / jnp.where(block_sum > 0, block_sum, 1.0)).astype(BF16)
    diag = iota((rows, 128), 0) == iota((rows, 128), 1)
    max_row = jnp.sum(jnp.where(diag, block_max, 0.0), axis=0, keepdims=True)
    sum_row = jnp.sum(jnp.where(diag, block_sum, 0.0), axis=0, keepdims=True)
    st_own[...] = jnp.where(iota((8, 128), 0) == 0, max_row, sum_row)
    bo_copies = [send("kv", d, bo_own, bo_in.at[d - 1]) for d in range(1, n_kv)]
    st_copies = [send("kv", d, st_own, st_in.at[d - 1]) for d in range(1, n_kv)]

    self_score = (
        jnp.sum(q_all[:, :rank] * latent_rows, axis=1, keepdims=True)
        + jnp.sum(q_all[:, rank:] * key_rows, axis=1, keepdims=True)
    ) * score_scale
    arrive(st_copies)
    maxes, sums = [block_max], [block_sum]
    for d in range(n_kv - 1):
        maxes.append(jnp.sum(jnp.where(diag, st_in[d, 0:1, :], 0.0), axis=1, keepdims=True))
        sums.append(jnp.sum(jnp.where(diag, st_in[d, 1:2, :], 0.0), axis=1, keepdims=True))
    top = self_score
    for one in maxes:
        top = jnp.maximum(top, one)
    weights = [total * jnp.exp(one - top) for one, total in zip(maxes, sums)]
    self_weight = jnp.exp(self_score - top)
    whole = self_weight
    for one in weights:
        whole = whole + one
    blend = self_weight * latent_rows + weights[0] * bo_own[...].astype(F32)
    for d in range(n_kv - 1):
        bo_copies[d].wait_recv()
        blend = blend + weights[d + 1] * bo_in[d].astype(F32)
    o_own[...] = (blend / whole).reshape(n_tp, group, rank).astype(BF16)
    o_copies = [
        send("tp", d, o_own.at[peer("tp", d)], o_in.at[tp]) for d in range(1, n_tp)
    ]
    o_in[tp] = o_own[tp]
    loads["vup"].wait()
    loads["out"].wait()
    arrive(o_copies)
    o_low = o_in[...].astype(F32).reshape(rows, rank).astype(BF16)
    v_cols = iota((rows, heads * VD), 1) // VD == iota((rows, heads * VD), 0) % heads
    v_wide = jnp.where(v_cols, dot(o_low, w_vup[...]), 0.0).astype(BF16)
    head_out = dot(gather, v_wide).astype(BF16)

    attn = dot(head_out, w_out[...])
    for i in range(n_tp):
        ap_own[i] = attn[:, i * col : (i + 1) * col].astype(BF16)
    ap_copies = [
        send("tp", d, ap_own.at[peer("tp", d)], ap_in.at[d - 1]) for d in range(1, n_tp)
    ]
    resid = tok_ref[...].astype(F32) + ap_own[tp].astype(F32)
    for d in range(n_tp - 1):
        ap_copies[d].wait_recv()
        resid = resid + ap_in[d].astype(F32)
    res_own[...] = resid.astype(BF16)
    res_copies = [send("tp", d, res_own, res_all.at[tp]) for d in range(1, n_tp)]
    resid = res_own[...].astype(F32)
    res_all[tp] = res_own[...]
    loads["up"].wait()
    arrive(res_copies)
    wide2 = jnp.concatenate([res_all[i] for i in range(n_tp)], axis=1).astype(F32)
    sq2_own[...] = jnp.broadcast_to(jnp.sum(wide2 * wide2, axis=1, keepdims=True), sq2_own.shape)
    scaled2 = (wide2 * gain_mlp[...]).astype(BF16)
    sq2_copies = [send("kv", d, sq2_own, sq2_in.at[d - 1]) for d in range(1, n_kv)]
    share = w_up.shape[1] // n_kv
    up_copies = []
    for d in range(1, n_kv):
        cols = pl.ds(pl.multiple_of(peer("kv", d) * share, 128), share)
        up_own[d - 1] = dot(scaled2, w_up[:, cols]).astype(BF16)
        up_copies.append(send("kv", d, up_own.at[d - 1], up_in.at[d - 1]))
    up_sum = dot(scaled2, w_up[:, pl.ds(pl.multiple_of(kv * share, 128), share)])
    for d in range(n_kv - 1):
        up_copies[d].wait_recv()
        up_sum = up_sum + up_in[d].astype(F32)
    act_own[...] = jnp.square(jnp.maximum(up_sum, 0.0)).astype(BF16)
    act_copies = [send("kv", d, act_own, act_all.at[d - 1]) for d in range(1, n_kv)]
    loads["down"].wait()
    down = dot(act_own[...], w_down[pl.ds(pl.multiple_of(kv * share, 128), share), :])
    for d in range(1, n_kv):
        act_copies[d - 1].wait_recv()
        source = lax.rem(kv + n_kv - d, n_kv)
        down = down + dot(
            act_all[d - 1], w_down[pl.ds(pl.multiple_of(source * share, 128), share), :]
        )
    for i in range(n_tp):
        dn_own[i] = down[:, i * col : (i + 1) * col].astype(BF16)
    dn_copies = [
        send("tp", d, dn_own.at[peer("tp", d)], dn_in.at[d - 1]) for d in range(1, n_tp)
    ]
    arrive(sq2_copies)
    square2 = sq2_own[:, 0:1]
    for d in range(n_kv - 1):
        square2 = square2 + sq2_in[d, :, 0:1]
    inv2 = lax.rsqrt(square2 / D + EPS)
    total = dn_own[tp].astype(F32)
    for d in range(n_tp - 1):
        dn_copies[d].wait_recv()
        total = total + dn_in[d].astype(F32)
    out_ref[...] = (resid + (inv2 * inv2) * total).astype(BF16)
    for copy in started:
        copy.wait_send()


def fused(
    n_kv,
    n_tp,
    tokens,
    lengths,
    gain_attn,
    w_query_nope,
    w_query_rope,
    w_latent,
    w_rope_key,
    gain_latent,
    w_key_up,
    w_value_up,
    w_out,
    gain_mlp,
    w_up,
    w_down,
    cache_latent,
    cache_rope,
):
    batch, col = tokens.shape
    seqs, cache_dev, rank = cache_latent.shape
    heads = w_key_up.shape[1] // NOPE
    rows, group = batch * heads, seqs * heads
    share = w_up.shape[1] // n_kv
    half = ROPE // 2
    freq = np.float32(10000.0) ** (-np.arange(half, dtype=np.float32) / np.float32(half))
    freq = freq.astype(np.float64)
    lanes = np.tile(freq, 2)[None, :]
    coarse = np.arange(n_kv * cache_dev // FINE)[:, None] * FINE * lanes
    fine = np.arange(FINE)[:, None] * lanes
    coarse = jnp.asarray(np.stack([np.cos(coarse), np.sin(coarse)]), F32)
    fine = jnp.asarray(np.stack([np.cos(fine), np.sin(fine)]), F32)
    wide_lanes = max(heads * ROPE, 128)
    freq_row = jnp.asarray(np.tile(np.tile(freq, wide_lanes // half)[None, :], (8, 1)), F32)

    def vm(*shape, kind=BF16):
        return pltpu.VMEM(shape, kind)

    weights = (
        w_query_nope,
        w_query_rope,
        w_latent,
        w_rope_key,
        w_key_up,
        w_value_up,
        w_out,
        w_up,
        w_down,
        cache_latent,
        cache_rope,
    )
    k, t = n_kv - 1, n_tp - 1
    qp = heads * (NOPE + ROPE)
    scratch = [vm(*w.shape, kind=w.dtype) for w in weights] + [
        vm(*cache_rope.shape),
        vm(n_tp, batch, col),
        vm(batch, qp),
        vm(k, batch, qp),
        vm(group, rank + 2 * ROPE, kind=F32),
        vm(k, group, rank + 2 * ROPE, kind=F32),
        vm(batch, 128, kind=F32),
        vm(k, batch, 128, kind=F32),
        vm(n_tp, group, rank + 128),
        vm(n_tp, group, rank + 128),
        vm(rows, rank),
        vm(k, rows, rank),
        vm(8, 128, kind=F32),
        vm(k, 8, 128, kind=F32),
        vm(n_tp, group, rank),
        vm(n_tp, group, rank),
        vm(n_tp, batch, col),
        vm(t, batch, col),
        vm(batch, col),
        vm(n_tp, batch, col),
        vm(k, batch, share),
        vm(k, batch, share),
        vm(batch, 128, kind=F32),
        vm(k, batch, 128, kind=F32),
        vm(batch, share),
        vm(k, batch, share),
        vm(n_tp, batch, col),
        vm(t, batch, col),
        pltpu.SemaphoreType.DMA((len(weights),)),
        pltpu.SemaphoreType.DMA((6 * t + 8 * k,)),
        pltpu.SemaphoreType.DMA((6 * t + 8 * k,)),
    ]
    in_vmem = pl.BlockSpec(memory_space=pltpu.VMEM)
    return pl.pallas_call(
        functools.partial(layer_kernel, n_kv, n_tp),
        out_shape=jax.ShapeDtypeStruct((batch, col), BF16),
        in_specs=[pl.BlockSpec(memory_space=pltpu.SMEM)]
        + [in_vmem] * 7
        + [pl.BlockSpec(memory_space=pl.ANY)] * len(weights),
        out_specs=in_vmem,
        scratch_shapes=scratch,
        compiler_params=pltpu.CompilerParams(
            collective_id=0, has_side_effects=True, vmem_limit_bytes=58 * 1024 * 1024
        ),
    )(
        lengths,
        tokens,
        gain_attn[None, :],
        gain_latent[None, :],
        gain_mlp[None, :],
        coarse,
        fine,
        freq_row,
        *weights,
    )


def solution(mesh):
    n_kv, n_tp = mesh.shape["kv"], mesh.shape["tp"]

    def step(*args):
        batch = args[0].shape[0]
        seqs = args[-1].shape[0]
        group = seqs * (args[8].shape[1] // NOPE)
        if group % 8 == 0 and group * n_tp <= 128 and batch % 16 == 0:
            return fused(n_kv, n_tp, *args)
        return per_device(*args)

    in_specs = (
        P(None, ("kv", "tp")),
        P(),
        P("kv"),
        P("kv", "tp"),
        P("kv", "tp"),
        P("kv", None),
        P("kv", None),
        P(),
        P(None, "tp"),
        P(None, "tp"),
        P("tp", "kv"),
        P("kv"),
        P("kv", "tp"),
        P("tp", "kv"),
        P("tp", "kv", None),
        P("tp", "kv", None),
    )
    out_specs = P(None, ("kv", "tp"))
    return jax.shard_map(
        step, mesh=mesh, in_specs=in_specs, out_specs=out_specs, check_vma=False
    )
```

```python
import functools

import jax
import jax.numpy as jnp
import numpy as np
from jax import lax
from jax.experimental import pallas as pl
from jax.experimental.pallas import tpu as pltpu
from jax.sharding import PartitionSpec as P

D = 4096
NOPE = 128
ROPE = 64
VD = 128
RANK = 512


EPS = 1e-06


def merged_2(value, axis, combine):
    everything = jax.tree.map(
        lambda part, kind: lax.all_gather(part.astype(kind), axis),
        value,
        (jnp.bfloat16, jnp.bfloat16, jnp.bfloat16),
    )

    def take(k):
        return jax.tree.map(lambda part, own: part[k].astype(own.dtype), everything, value)

    return lax.fori_loop(
        1, lax.axis_size(axis), lambda k, so_far: combine(so_far, take(k)), take(0)
    )


def rotate(values, positions):
    half_dim = values.shape[-1] // 2
    inv_freq = 10000.0 ** (-jnp.arange(half_dim, dtype=jnp.float32) / half_dim)
    angles = positions.astype(jnp.float32)[..., None] * inv_freq
    cos_part = jnp.cos(angles)
    sin_part = jnp.sin(angles)
    lower = values[..., :half_dim]
    upper = values[..., half_dim:]
    return jnp.concatenate(
        [lower * cos_part - upper * sin_part, upper * cos_part + lower * sin_part], axis=-1
    )


def combine(earlier, later):
    max_one, sum_one, out_one = earlier
    max_two, sum_two, out_two = later
    new_max = jnp.maximum(max_one, max_two)
    weight_one = sum_one * jnp.exp(max_one - new_max)
    weight_two = sum_two * jnp.exp(max_two - new_max)
    merged = weight_one + weight_two
    safe_sum = jnp.where(merged > 0, merged, 1.0)
    result = (
        weight_one[..., None] * out_one.astype(jnp.float32)
        + weight_two[..., None] * out_two.astype(jnp.float32)
    ) / safe_sum[..., None]
    return (new_max, merged, result.astype(jnp.bfloat16))


def per_device(
    tokens,
    lengths,
    gain_attn,
    w_query_nope,
    w_query_rope,
    w_latent,
    w_rope_key,
    gain_latent,
    w_key_up,
    w_value_up,
    w_out,
    gain_mlp,
    w_up,
    w_down,
    cache_latent,
    cache_rope,
):
    kv_index = lax.axis_index("kv")
    tp_index = lax.axis_index("tp")
    seq_dev = cache_latent.shape[0]
    cache_dev = cache_latent.shape[1]
    heads_dev = w_key_up.shape[1] // NOPE
    block_cols = lax.all_gather(tokens, "tp", axis=1, tiled=True)
    batch_rows = block_cols.shape[0]
    widened = block_cols.astype(jnp.float32)
    square_piece = jnp.sum(widened * widened, axis=1)
    scaled = (widened * gain_attn).astype(jnp.bfloat16)
    part_nope = jnp.dot(scaled, w_query_nope, preferred_element_type=jnp.float32)
    part_rope = jnp.dot(scaled, w_query_rope, preferred_element_type=jnp.float32)
    own_rows = lax.dynamic_slice_in_dim(scaled, tp_index * seq_dev, seq_dev, 0)
    part_latent = jnp.dot(own_rows, w_latent, preferred_element_type=jnp.float32)
    part_key = jnp.dot(own_rows, w_rope_key, preferred_element_type=jnp.float32)
    square_sum, nope_sum, rope_sum, latent_sum, key_sum = lax.psum(
        (square_piece, part_nope, part_rope, part_latent, part_key), "kv"
    )
    inv_rms = lax.rsqrt(square_sum / D + EPS)
    q_nope = (nope_sum * inv_rms[:, None]).astype(jnp.bfloat16).reshape(batch_rows, heads_dev, NOPE)
    rope_raw = (rope_sum * inv_rms[:, None]).reshape(batch_rows, heads_dev, ROPE)
    q_rope = rotate(rope_raw, lengths[:, None]).astype(jnp.bfloat16)
    key_up = w_key_up.reshape(RANK, heads_dev, NOPE)
    q_latent = jnp.einsum(
        "bhn,rhn->bhr", q_nope, key_up, preferred_element_type=jnp.float32
    ).astype(jnp.bfloat16)
    latent_query, rope_query = (
        lax.all_to_all(q_latent, "tp", split_axis=0, concat_axis=1, tiled=True),
        lax.all_to_all(q_rope, "tp", split_axis=0, concat_axis=1, tiled=True),
    )
    own_inv = lax.dynamic_slice_in_dim(inv_rms, tp_index * seq_dev, seq_dev, 0)
    own_len = lax.dynamic_slice_in_dim(lengths, tp_index * seq_dev, seq_dev, 0)
    raw_latent = latent_sum * own_inv[:, None]
    latent_new = (
        raw_latent
        * lax.rsqrt(jnp.mean(raw_latent * raw_latent, axis=1, keepdims=True) + EPS)
        * gain_latent
    ).astype(jnp.bfloat16)
    key_new = rotate(key_sum * own_inv[:, None], own_len).astype(jnp.bfloat16)
    score_scale = (NOPE + ROPE) ** (-0.5)
    positions = kv_index * cache_dev + jnp.arange(cache_dev, dtype=jnp.int32)
    rotated = rotate(cache_rope.astype(jnp.float32), positions).astype(jnp.bfloat16)
    scores = (
        jnp.einsum("shr,spr->shp", latent_query, cache_latent, preferred_element_type=jnp.float32)
        + jnp.einsum("shk,spk->shp", rope_query, rotated, preferred_element_type=jnp.float32)
    ) * score_scale
    live_mask = positions[None, None, :] < own_len[:, None, None]
    block_max = jnp.max(jnp.where(live_mask, scores, -1e30), axis=2)
    exponent = jnp.where(live_mask, jnp.exp(scores - block_max[..., None]), 0.0)
    block_sum = jnp.sum(exponent, axis=2)
    weighted = jnp.einsum(
        "shp,spr->shr",
        exponent.astype(jnp.bfloat16),
        cache_latent,
        preferred_element_type=jnp.float32,
    )
    block_out = (weighted / jnp.where(block_sum > 0, block_sum, 1.0)[..., None]).astype(
        jnp.bfloat16
    )
    block_max, block_sum, block_out = merged_2((block_max, block_sum, block_out), "kv", combine)
    own_score = (
        jnp.einsum("shr,sr->sh", latent_query, latent_new, preferred_element_type=jnp.float32)
        + jnp.einsum("shk,sk->sh", rope_query, key_new, preferred_element_type=jnp.float32)
    ) * score_scale
    new_max = jnp.maximum(block_max, own_score)
    carried = block_sum * jnp.exp(block_max - new_max)
    own_weight = jnp.exp(own_score - new_max)
    o_latent = (
        (
            carried[..., None] * block_out.astype(jnp.float32)
            + own_weight[..., None] * latent_new.astype(jnp.float32)[:, None, :]
        )
        / (carried + own_weight)[..., None]
    ).astype(jnp.bfloat16)
    head_latent = lax.all_to_all(o_latent, "tp", split_axis=1, concat_axis=0, tiled=True)
    value_up = w_value_up.reshape(RANK, heads_dev, VD)
    head_out = (
        jnp.einsum("bhr,rhv->bhv", head_latent, value_up, preferred_element_type=jnp.float32)
        .astype(jnp.bfloat16)
        .reshape(batch_rows, heads_dev * VD)
    )
    attn_part = jnp.dot(head_out, w_out, preferred_element_type=jnp.float32)
    attn_sum = lax.psum(attn_part, "tp")
    resid = (widened + attn_sum).astype(jnp.bfloat16)
    resid_wide = resid.astype(jnp.float32)
    square_two = jnp.sum(resid_wide * resid_wide, axis=1)
    scaled2 = (resid_wide * gain_mlp).astype(jnp.bfloat16)
    up_part = jnp.dot(scaled2, w_up, preferred_element_type=jnp.float32)
    spread_squares = jnp.broadcast_to(square_two[:, None], (batch_rows, lax.axis_size("kv")))
    up_share, square_cols = (
        lax.psum_scatter(up_part, "kv", scatter_dimension=1, tiled=True),
        lax.psum_scatter(spread_squares, "kv", scatter_dimension=1, tiled=True),
    )
    square_all = square_cols[:, 0]
    active_share = jnp.square(jnp.maximum(up_share, 0.0)).astype(jnp.bfloat16)
    activated = lax.all_gather(active_share, "kv", axis=1, tiled=True)
    inv_rms2 = lax.rsqrt(square_all / D + EPS)
    down_part = jnp.dot(activated, w_down, preferred_element_type=jnp.float32)
    down_sum = lax.psum_scatter(down_part, "tp", scatter_dimension=1, tiled=True)
    out_cols = down_sum.shape[1]
    resid_cols = lax.dynamic_slice_in_dim(resid_wide, tp_index * out_cols, out_cols, 1)
    return (resid_cols + (inv_rms2 * inv_rms2)[:, None] * down_sum).astype(jnp.bfloat16)


MESH = pl.DeviceIdType.MESH
BF16 = jnp.bfloat16
F32 = jnp.float32


def dot(a, b):
    return jnp.dot(a, b, preferred_element_type=F32)


def dot_nt(a, b):
    return lax.dot_general(a, b, (((1,), (1,)), ((), ())), preferred_element_type=F32)


def iota(shape, axis):
    return lax.broadcasted_iota(jnp.int32, shape, axis)


def layer_kernel(
    n_kv,
    n_tp,
    len_ref,
    tok_ref,
    gain_attn,
    gain_latent,
    gain_mlp,
    freq_ref,
    h_turn,
    h_qn,
    h_qr,
    h_lat,
    h_key,
    h_kup,
    h_vup,
    h_out,
    h_up,
    h_down,
    h_cl,
    h_cr,
    out_ref,
    w_qn,
    w_qr,
    w_lat,
    w_key,
    w_kup,
    w_vup,
    w_out,
    w_up,
    w_down,
    c_lat,
    c_rope,
    turn,
    rot,
    tok_all,
    qp_own,
    qp_in,
    lat_own,
    lat_in,
    sq_own,
    sq_in,
    q_own,
    q_in,
    bo_own,
    bo_in,
    st_own,
    st_in,
    o_own,
    o_in,
    ap_own,
    ap_in,
    res_own,
    res_all,
    up_own,
    up_in,
    sq2_own,
    sq2_in,
    dn_own,
    dn_in,
    load_sem,
    send_sem,
    recv_sem,
):
    kv = lax.axis_index("kv")
    tp = lax.axis_index("tp")
    size = {"kv": n_kv, "tp": n_tp}
    here = {"kv": kv, "tp": tp}
    batch, col = tok_ref.shape
    seqs, cache_dev, rank = c_lat.shape
    heads = w_kup.shape[1] // NOPE
    rows = batch * heads
    group = seqs * heads
    n_nope = heads * NOPE
    n_rope = heads * ROPE

    loads = {}
    order = (
        ("qn", h_qn, w_qn),
        ("qr", h_qr, w_qr),
        ("lat", h_lat, w_lat),
        ("key", h_key, w_key),
        ("turn", h_turn.at[kv], turn),
        ("cr", h_cr, c_rope),
        ("kup", h_kup, w_kup),
        ("cl", h_cl, c_lat),
        ("vup", h_vup, w_vup),
        ("out", h_out, w_out),
        ("up", h_up, w_up),
        ("down", h_down, w_down),
    )
    for i, (name, hbm, vmem) in enumerate(order):
        loads[name] = pltpu.make_async_copy(hbm, vmem, load_sem.at[i])
        loads[name].start()

    barrier = pltpu.get_barrier_semaphore()
    for axis in ("kv", "tp"):
        for d in range(1, size[axis]):
            pl.semaphore_signal(
                barrier,
                inc=1,
                device_id={axis: lax.rem(here[axis] + d, size[axis])},
                device_id_type=MESH,
            )

    started = []

    def send(axis, d, source, target):
        return send_to({axis: peer(axis, d)}, source, target)

    def send_to(device, source, target):
        i = len(started)
        copy = pltpu.make_async_remote_copy(
            src_ref=source,
            dst_ref=target,
            send_sem=send_sem.at[i],
            recv_sem=recv_sem.at[i],
            device_id=device,
            device_id_type=MESH,
        )
        copy.start()
        started.append(copy)
        return copy

    def peer(axis, d):
        return lax.rem(here[axis] + d, size[axis])

    def arrive(copies):
        for copy in copies:
            copy.wait_recv()

    lane_r = iota((batch, n_rope), 1)
    row_b = iota((batch, n_rope), 0)
    len_b = jnp.zeros((batch, n_rope), jnp.int32)
    for b in range(batch):
        len_b = jnp.where(row_b == b, len_ref[b], len_b)
    angle = len_b.astype(F32) * freq_ref[0:1, :n_rope]
    q_cos = jnp.cos(angle)
    q_sin = jnp.sin(angle)
    lane_k = iota((group, 128), 1)
    row_k = iota((group, 128), 0) // heads
    len_k = jnp.zeros((group, 128), jnp.int32)
    for s in range(seqs):
        len_k = jnp.where(row_k == s, len_ref[tp * seqs + s], len_k)
    angle_k = len_k.astype(F32) * freq_ref[0:1, :128]
    k_cos = jnp.cos(angle_k)
    k_sin = jnp.sin(angle_k)

    spread = (iota((rows, batch), 0) // heads == iota((rows, batch), 1)).astype(F32).astype(BF16)
    gather = (iota((batch, rows), 1) // heads == iota((batch, rows), 0)).astype(F32).astype(BF16)
    pick = (iota((group, batch), 0) // heads + tp * seqs == iota((group, batch), 1))
    pick = pick.astype(F32).astype(BF16)

    pl.semaphore_wait(barrier, n_kv + n_tp - 2)

    tok_copies = [send("tp", d, tok_ref, tok_all.at[tp]) for d in range(1, n_tp)]
    tok_all[tp] = tok_ref[...]

    loads["turn"].wait()
    loads["cr"].wait()
    half = ROPE // 2
    key_cos, key_sin = turn[0], turn[1]
    for s in range(seqs):
        lower = c_rope[s, :half].astype(F32)
        upper = c_rope[s, half:].astype(F32)
        rot[s, :half] = (lower * key_cos - upper * key_sin).astype(BF16)
        rot[s, half:] = (upper * key_cos + lower * key_sin).astype(BF16)

    arrive(tok_copies)
    toks = jnp.concatenate([tok_all[i] for i in range(n_tp)], axis=1)
    wide = toks.astype(F32)
    scaled = (wide * gain_attn[...]).astype(BF16)
    loads["qn"].wait()
    qp_own[:, :n_nope] = dot(scaled, w_qn[...]).astype(BF16)
    loads["qr"].wait()
    qp_own[:, n_nope:] = dot(scaled, w_qr[...]).astype(BF16)
    sq_own[...] = jnp.broadcast_to(jnp.sum(wide * wide, axis=1, keepdims=True), sq_own.shape)
    qp_copies = [send("kv", d, qp_own, qp_in.at[d - 1]) for d in range(1, n_kv)]
    sq_copies = [send("kv", d, sq_own, sq_in.at[d - 1]) for d in range(1, n_kv)]
    own_tok = dot(pick, toks)
    own_scaled = (own_tok * gain_attn[...]).astype(BF16)
    loads["lat"].wait()
    lat_own[:, :rank] = dot(own_scaled, w_lat[...])
    loads["key"].wait()
    lat_own[:, rank : rank + ROPE] = dot_nt(own_scaled, w_key[...])
    lat_own[:, rank + ROPE :] = jnp.broadcast_to(
        jnp.sum(own_tok * own_tok, axis=1, keepdims=True), (group, ROPE)
    )
    lat_copies = [send("kv", d, lat_own, lat_in.at[d - 1]) for d in range(1, n_kv)]

    loads["kup"].wait()
    arrive(qp_copies)
    arrive(sq_copies)
    q_sum = qp_own[...].astype(F32)
    square = sq_own[:, 0:1]
    for d in range(n_kv - 1):
        q_sum = q_sum + qp_in[d].astype(F32)
        square = square + sq_in[d, :, 0:1]
    q_sum = q_sum * lax.rsqrt(square / D + EPS)
    q_nope = q_sum[:, :n_nope].astype(BF16)
    raw = q_sum[:, n_nope:]
    swapped = jnp.where(
        lane_r % ROPE < half, -pltpu.roll(raw, n_rope - half, 1), pltpu.roll(raw, half, 1)
    )
    q_rope = (raw * q_cos + swapped * q_sin).astype(BF16)
    own_cols = iota((rows, n_nope), 1) // NOPE == iota((rows, n_nope), 0) % heads
    own_rope = iota((rows, n_rope), 1) // ROPE == iota((rows, n_rope), 0) % heads
    q_wide = jnp.where(own_cols, dot(spread, q_nope), 0.0).astype(BF16)
    q_lat = dot_nt(q_wide, w_kup[...])
    r_wide = jnp.where(own_rope, dot(spread, q_rope), 0.0).astype(BF16)
    fold = (iota((n_rope, 128), 0) % ROPE == iota((n_rope, 128), 1)).astype(F32).astype(BF16)
    q_rot = dot(r_wide, fold)
    q_own[:, :, :rank] = q_lat.reshape(n_tp, group, rank).astype(BF16)
    q_own[:, :, rank:] = q_rot.reshape(n_tp, group, 128).astype(BF16)
    q_copies = [
        send("tp", d, q_own.at[peer("tp", d)], q_in.at[tp]) for d in range(1, n_tp)
    ]
    q_in[tp] = q_own[tp]

    arrive(lat_copies)
    lat_sum = lat_own[...]
    for d in range(n_kv - 1):
        lat_sum = lat_sum + lat_in[d]
    own_inv = lax.rsqrt(lat_sum[:, rank + ROPE : rank + ROPE + 1] / D + EPS)
    raw_latent = lat_sum[:, :rank] * own_inv
    mean_sq = jnp.mean(raw_latent * raw_latent, axis=1, keepdims=True)
    latent_new = (raw_latent * lax.rsqrt(mean_sq + EPS) * gain_latent[...]).astype(BF16).astype(F32)
    raw_key = lat_sum[:, rank:] * own_inv
    raw_key = jnp.where(lane_k < ROPE, raw_key, pltpu.roll(raw_key, ROPE, 1))
    swap_key = jnp.where(
        lane_k % ROPE < half, -pltpu.roll(raw_key, 128 - half, 1), pltpu.roll(raw_key, half, 1)
    )
    key_new = (raw_key * k_cos + swap_key * k_sin).astype(BF16).astype(F32)
    key_new = jnp.where(lane_k < ROPE, key_new, 0.0)
    latent_rows = jnp.broadcast_to(latent_new[None], (n_tp, group, rank)).reshape(rows, rank)
    key_rows = jnp.broadcast_to(key_new[None], (n_tp, group, 128)).reshape(rows, 128)

    row_seq = iota((rows, 1), 0) % group // heads
    own_len = jnp.zeros((rows, 1), jnp.int32)
    for s in range(seqs):
        own_len = jnp.where(row_seq == s, len_ref[tp * seqs + s], own_len)
    score_scale = (NOPE + ROPE) ** (-0.5)

    loads["cl"].wait()
    arrive(q_copies)
    q_all = q_in[...].astype(F32).reshape(rows, rank + 128)
    q_low = q_all.astype(BF16)
    latent_query = q_low[:, :rank]
    rope_query = q_low[:, rank : rank + ROPE]
    scores = None
    for s in range(seqs):
        one = dot_nt(latent_query, c_lat[s]) + dot(rope_query, rot[s])
        scores = one if scores is None else jnp.where(row_seq == s, one, scores)
    scores = scores * score_scale
    live = kv * cache_dev + iota((rows, cache_dev), 1) < own_len
    block_max = jnp.max(jnp.where(live, scores, -1e30), axis=1, keepdims=True)
    expo = jnp.where(live, jnp.exp(scores - block_max), 0.0)
    block_sum = jnp.sum(expo, axis=1, keepdims=True)
    expo_low = expo.astype(BF16)
    weighted = None
    for s in range(seqs):
        one = dot(expo_low, c_lat[s])
        weighted = one if weighted is None else jnp.where(row_seq == s, one, weighted)
    bo_own[...] = (weighted / jnp.where(block_sum > 0, block_sum, 1.0)).astype(BF16)
    diag = iota((rows, 128), 0) == iota((rows, 128), 1)
    max_row = jnp.sum(jnp.where(diag, block_max, 0.0), axis=0, keepdims=True)
    sum_row = jnp.sum(jnp.where(diag, block_sum, 0.0), axis=0, keepdims=True)
    half_z, core = tp // 2, lax.rem(tp, 2)
    n_z, part_rows = n_tp // 2, 2 * group
    parts = list(range(n_z // 2, n_z)) + list(range(1, n_z // 2)) + [0]
    parts = list(dict.fromkeys(parts))
    st_own[...] = jnp.where(iota((8, 128), 0) == 0, max_row, sum_row)
    st_copies = [send("kv", d, st_own, st_in.at[d - 1]) for d in range(1, n_kv)]
    part_of, bo_copies = {}, {}
    for dz in parts:
        part_of[dz] = lax.rem(half_z + dz, n_z)
        span = pl.ds(pl.multiple_of(part_of[dz] * part_rows, 16), part_rows)
        bo_copies[dz] = [
            send("kv", d, bo_own.at[span], bo_in.at[d - 1, span]) for d in range(1, n_kv)
        ]

    self_score = (
        jnp.sum(q_all[:, :rank] * latent_rows, axis=1, keepdims=True)
        + jnp.sum(q_all[:, rank:] * key_rows, axis=1, keepdims=True)
    ) * score_scale
    self_row = jnp.sum(jnp.where(diag, self_score, 0.0), axis=0, keepdims=True)
    arrive(st_copies)
    max_rows = [max_row] + [st_in[d, 0:1, :] for d in range(n_kv - 1)]
    sum_rows = [sum_row] + [st_in[d, 1:2, :] for d in range(n_kv - 1)]
    top = self_row
    for one in max_rows:
        top = jnp.maximum(top, one)
    weight_rows = [total * jnp.exp(one - top) for one, total in zip(max_rows, sum_rows)]
    weight_rows.append(jnp.exp(self_row - top))
    whole_row = weight_rows[0]
    for one in weight_rows[1:]:
        whole_row = whole_row + one
    o_copies = []
    for dz in parts:
        at = part_of[dz]
        span = pl.ds(pl.multiple_of(at * part_rows, 16), part_rows)
        mine = iota((part_rows, 128), 0) + at * part_rows == iota((part_rows, 128), 1)

        def column(row):
            return jnp.sum(jnp.where(mine, row, 0.0), axis=1, keepdims=True)

        arrive(bo_copies[dz])
        blend = column(weight_rows[-1]) * latent_rows[:part_rows]
        blend = blend + column(weight_rows[0]) * bo_own[span, :].astype(F32)
        for d in range(n_kv - 1):
            blend = blend + column(weight_rows[d + 1]) * bo_in[d, span, :].astype(F32)
        blend = (blend / column(whole_row)).reshape(2, group, rank)
        o_own[pl.ds(2 * at, 2)] = blend.astype(BF16)
        for dc in range(2):
            target = 2 * at + lax.rem(core + dc, 2)
            if dz == 0 and dc == 0:
                o_in[tp] = o_own[tp]
            else:
                o_copies.append(send_to({"tp": target}, o_own.at[target], o_in.at[tp]))
    loads["vup"].wait()
    loads["out"].wait()
    arrive(o_copies)
    o_low = o_in[...].astype(F32).reshape(rows, rank).astype(BF16)
    v_cols = iota((rows, heads * VD), 1) // VD == iota((rows, heads * VD), 0) % heads
    v_wide = jnp.where(v_cols, dot(o_low, w_vup[...]), 0.0).astype(BF16)
    head_out = dot(gather, v_wide).astype(BF16)

    attn = dot(head_out, w_out[...])
    for i in range(n_tp):
        ap_own[i] = attn[:, i * col : (i + 1) * col].astype(BF16)
    ap_copies = [
        send("tp", d, ap_own.at[peer("tp", d)], ap_in.at[d - 1]) for d in range(1, n_tp)
    ]
    resid = tok_ref[...].astype(F32) + ap_own[tp].astype(F32)
    for d in range(n_tp - 1):
        ap_copies[d].wait_recv()
        resid = resid + ap_in[d].astype(F32)
    res_own[...] = resid.astype(BF16)
    res_copies = [send("tp", d, res_own, res_all.at[tp]) for d in range(1, n_tp)]
    resid = res_own[...].astype(F32)
    res_all[tp] = res_own[...]
    loads["up"].wait()
    arrive(res_copies)
    wide2 = jnp.concatenate([res_all[i] for i in range(n_tp)], axis=1).astype(F32)
    sq2_own[...] = jnp.broadcast_to(jnp.sum(wide2 * wide2, axis=1, keepdims=True), sq2_own.shape)
    scaled2 = (wide2 * gain_mlp[...]).astype(BF16)
    sq2_copies = [send("kv", d, sq2_own, sq2_in.at[d - 1]) for d in range(1, n_kv)]
    share = w_up.shape[1] // n_kv
    up_copies = []
    for i in range(n_kv):
        up_own[i] = dot(scaled2, w_up[:, i * share : (i + 1) * share]).astype(BF16)
        up_copies.append([send("kv", d, up_own.at[i], up_in.at[d - 1, i]) for d in range(1, n_kv)])
    loads["down"].wait()
    down = jnp.zeros((batch, w_down.shape[1]), F32)
    for i in range(n_kv):
        arrive(up_copies[i])
        up_sum = up_own[i].astype(F32)
        for d in range(n_kv - 1):
            up_sum = up_sum + up_in[d, i].astype(F32)
        active = jnp.square(jnp.maximum(up_sum, 0.0)).astype(BF16)
        down = down + dot(active, w_down[i * share : (i + 1) * share, :])
    for i in range(n_tp):
        dn_own[i] = down[:, i * col : (i + 1) * col].astype(BF16)
    dn_copies = [
        send("tp", d, dn_own.at[peer("tp", d)], dn_in.at[d - 1]) for d in range(1, n_tp)
    ]
    arrive(sq2_copies)
    square2 = sq2_own[:, 0:1]
    for d in range(n_kv - 1):
        square2 = square2 + sq2_in[d, :, 0:1]
    inv2 = lax.rsqrt(square2 / D + EPS)
    total = dn_own[tp].astype(F32)
    for d in range(n_tp - 1):
        dn_copies[d].wait_recv()
        total = total + dn_in[d].astype(F32)
    out_ref[...] = (resid + (inv2 * inv2) * total).astype(BF16)
    for copy in started:
        copy.wait_send()


def fused(
    n_kv,
    n_tp,
    tokens,
    lengths,
    gain_attn,
    w_query_nope,
    w_query_rope,
    w_latent,
    w_rope_key,
    gain_latent,
    w_key_up,
    w_value_up,
    w_out,
    gain_mlp,
    w_up,
    w_down,
    cache_latent,
    cache_rope,
):
    batch, col = tokens.shape
    seqs, cache_dev, rank = cache_latent.shape
    heads = w_key_up.shape[1] // NOPE
    rows, group = batch * heads, seqs * heads
    share = w_up.shape[1] // n_kv
    half = ROPE // 2
    freq = np.float32(10000.0) ** (-np.arange(half, dtype=np.float32) / np.float32(half))
    angles = freq.astype(np.float64)[:, None] * np.arange(n_kv * cache_dev)
    turns = np.stack([np.cos(angles), np.sin(angles)]).reshape(2, half, n_kv, cache_dev)
    turns = jnp.asarray(turns.transpose(2, 0, 1, 3), F32)
    wide_lanes = max(heads * ROPE, 128)
    freq_row = jnp.asarray(np.tile(np.tile(freq, wide_lanes // half)[None, :], (8, 1)), F32)

    def vm(*shape, kind=BF16):
        return pltpu.VMEM(shape, kind)

    w_rope_key = w_rope_key.T
    cache_rope = jnp.swapaxes(cache_rope, 1, 2)
    weights = (
        w_query_nope,
        w_query_rope,
        w_latent,
        w_rope_key,
        w_key_up,
        w_value_up,
        w_out,
        w_up,
        w_down,
        cache_latent,
        cache_rope,
    )
    k, t = n_kv - 1, n_tp - 1
    qp = heads * (NOPE + ROPE)
    scratch = [vm(*w.shape, kind=w.dtype) for w in weights] + [
        vm(2, half, cache_dev, kind=F32),
        vm(*cache_rope.shape),
        vm(n_tp, batch, col),
        vm(batch, qp),
        vm(k, batch, qp),
        vm(group, rank + 2 * ROPE, kind=F32),
        vm(k, group, rank + 2 * ROPE, kind=F32),
        vm(batch, 128, kind=F32),
        vm(k, batch, 128, kind=F32),
        vm(n_tp, group, rank + 128),
        vm(n_tp, group, rank + 128),
        vm(rows, rank),
        vm(k, rows, rank),
        vm(8, 128, kind=F32),
        vm(k, 8, 128, kind=F32),
        vm(n_tp, group, rank),
        vm(n_tp, group, rank),
        vm(n_tp, batch, col),
        vm(t, batch, col),
        vm(batch, col),
        vm(n_tp, batch, col),
        vm(n_kv, batch, share),
        vm(k, n_kv, batch, share),
        vm(batch, 128, kind=F32),
        vm(k, batch, 128, kind=F32),
        vm(n_tp, batch, col),
        vm(t, batch, col),
        pltpu.SemaphoreType.DMA((len(weights) + 1,)),
        pltpu.SemaphoreType.DMA((6 * t + (5 + n_kv + n_tp // 2) * k,)),
        pltpu.SemaphoreType.DMA((6 * t + (5 + n_kv + n_tp // 2) * k,)),
    ]
    in_vmem = pl.BlockSpec(memory_space=pltpu.VMEM)
    return pl.pallas_call(
        functools.partial(layer_kernel, n_kv, n_tp),
        out_shape=jax.ShapeDtypeStruct((batch, col), BF16),
        in_specs=[pl.BlockSpec(memory_space=pltpu.SMEM)]
        + [in_vmem] * 5
        + [pl.BlockSpec(memory_space=pl.ANY)] * (1 + len(weights)),
        out_specs=in_vmem,
        scratch_shapes=scratch,
        compiler_params=pltpu.CompilerParams(
            collective_id=0, has_side_effects=True, vmem_limit_bytes=58 * 1024 * 1024
        ),
    )(
        lengths,
        tokens,
        gain_attn[None, :],
        gain_latent[None, :],
        gain_mlp[None, :],
        freq_row,
        turns,
        *weights,
    )


def solution(mesh):
    n_kv, n_tp = mesh.shape["kv"], mesh.shape["tp"]

    def step(*args):
        batch = args[0].shape[0]
        seqs = args[-1].shape[0]
        group = seqs * (args[8].shape[1] // NOPE)
        if group % 8 == 0 and group * n_tp <= 128 and batch % 16 == 0 and n_tp % 2 == 0:
            return fused(n_kv, n_tp, *args)
        return per_device(*args)

    in_specs = (
        P(None, ("kv", "tp")),
        P(),
        P("kv"),
        P("kv", "tp"),
        P("kv", "tp"),
        P("kv", None),
        P("kv", None),
        P(),
        P(None, "tp"),
        P(None, "tp"),
        P("tp", "kv"),
        P("kv"),
        P("kv", "tp"),
        P("tp", "kv"),
        P("tp", "kv", None),
        P("tp", "kv", None),
    )
    out_specs = P(None, ("kv", "tp"))
    return jax.shard_map(
        step, mesh=mesh, in_specs=in_specs, out_specs=out_specs, check_vma=False
    )
```
